256 devices in a mesh: sp: 32 (over z, y), tp: 8 (over x, core).
Axes of the slice: x: 4, y: 4, z: 8, core: 2. Of those that a mesh axis runs over, the one named last changes fastest.
Arguments:
- skip_trunk_vector: bfloat16 [16384, 2048], P('sp', 'tp'), may hold values from -16 to 16
- valve_preactivation: bfloat16 [16384, 2048], P('sp', 'tp'), may hold values from -6 to 6
- projected_heads_payload: bfloat16 [16384, 2048], P('sp', 'tp'), may hold values from -6 to 6
- cluster_ingests: bfloat16 [16384, 1024], P('sp', 'tp'), may hold values from -6 to 6
- cluster_observers: bfloat16 [16384, 1024], P('sp', 'tp'), may hold values from -6 to 6
- pre_softplus_increments: float32 [2, 16384, 32], P(None, 'sp', 'tp'), may hold values from -6 to 6
- attenuation_ln_rate: float32 [2, 32], P(None, 'tp'), may hold values from -13 to -3
- additional_attenuation: float32 [2, 16384, 32], P(None, 'sp', 'tp'), may hold values from -3 to 0
- payload_conv_weights: float32 [7, 2048], P(None, 'tp'), may hold values from -2 to 2
- ingest_conv_weights: float32 [7, 1024], P(None, 'tp'), may hold values from -2 to 2
- observer_conv_weights: float32 [7, 1024], P(None, 'tp'), may hold values from -2 to 2
- valved_cluster_factor: float32 [2048], P('tp'), may hold values from 0.1 to 1.9
- closing_map_matrix: bfloat16 [2048, 2048], P('tp'), may hold values from -0.125 to 0.125
- dense_standardize_factor: float32 [2048], replicated, may hold values from 0.1 to 1.9
- dense_valve_map: bfloat16 [2048, 5120], P('sp', 'tp'), may hold values from -0.125 to 0.125
- dense_payload_map: bfloat16 [2048, 5120], P('sp', 'tp'), may hold values from -0.125 to 0.125
- valve_series_smoother: float32 [3, 5120], P(None, 'tp'), may hold values from -3.5 to 3.5
- payload_series_smoother: float32 [3, 5120], P(None, 'tp'), may hold values from -3.5 to 3.5
- dense_contract_map: bfloat16 [5120, 2048], P('tp', 'sp'), may hold values from -0.078125 to 0.078125
Outputs:
- updated: bfloat16 [16384, 2048], P('sp', 'tp')
The draws below stay inside these ranges and needn't reach their ends.
All inputs are finite; a program needn't handle non-finite values.
Results may differ from the reference program's by a relative error of at most 0.019.
Values may be sent and summed in bfloat16 or wider, within the bound.
A program may use at most 64 MiB of HBM per device.

```python
import jax
import jax.numpy as jnp
from jax import lax

TOK_DEV = 512
D = 2048
HEADS = 32
HEAD_DIM = 64
GROUPS = 8
STATE = 128
CONV = 7
FF = 5120
FF_TAPS = 3
MIXING_WIDTH = 2048
SEQUENCE_SPAN = 16384
N_TP = 8


def draw_skip_trunk_vector(key, part):
    column = jnp.arange(D, dtype=jnp.float32) / D
    scales = 0.5 * jnp.exp(jnp.log(5.0) * column)
    random_part = jax.random.truncated_normal(key, -6.0, 6.0, (SEQUENCE_SPAN, D), jnp.float32)
    return (random_part * scales).astype(jnp.bfloat16)


def draw_pre_softplus_increments(key, part):
    key_one, key_two = jax.random.split(key)
    blocks = SEQUENCE_SPAN // TOK_DEV
    offsets = jax.random.uniform(key_two, (2, blocks, 1, HEADS), jnp.float32, -1.2, 1.2)
    spread = jnp.broadcast_to(offsets, (2, blocks, TOK_DEV, HEADS)).reshape(2, SEQUENCE_SPAN, HEADS)
    random_part = jax.random.truncated_normal(key_one, -4.0, 4.0, (2, SEQUENCE_SPAN, HEADS), jnp.float32)
    return random_part + spread


def draw_attenuation_ln_rate(key, part):
    key_one, key_two, key_three = jax.random.split(key, 3)
    quick = jax.random.bernoulli(key_one, 0.5, (2, HEADS))
    slow_rate = jax.random.uniform(key_two, (2, HEADS), jnp.float32, 0.5, 1.0) * (0.6 / SEQUENCE_SPAN)
    fast_rate = jnp.exp(jax.random.uniform(key_three, (2, HEADS), jnp.float32, jnp.log(1.0 / 60.0), jnp.log(1.0 / 25.0)))
    return jnp.log(jnp.where(quick, fast_rate, slow_rate))


def draw_additional_attenuation(key, part):
    key_one, key_two = jax.random.split(key)
    places = jax.random.randint(key_one, (2, 4), 0, SEQUENCE_SPAN)
    kept_share = jax.random.uniform(key_two, (2, 4, HEADS), jnp.float32, 0.5, 0.8)
    position = jnp.arange(SEQUENCE_SPAN, dtype=jnp.int32)
    matches = (position[None, :, None] == places[:, None, :]).astype(jnp.float32)
    return jnp.einsum('dtk,dkh->dth', matches, jnp.log(kept_share))


def level_of(stream_key, extent, cuts, low, top_value):
    def one(axis_at, parts):
        heights = jax.random.uniform(jax.random.fold_in(jax.random.fold_in(stream_key, 6), axis_at), (parts,), jnp.float32, low / len(cuts), top_value / len(cuts))
        return jnp.repeat(jnp.exp(heights), extent[axis_at] // parts).reshape((-1,) + (1,) * (len(extent) - axis_at - 1))

    level = one(*cuts[0])
    for cut in cuts[1:]:
        level = level * one(*cut)
    return level


def noise(stream_key, extent, width, limit, cuts=(), held_as=jnp.bfloat16):
    factor_of = level_of(stream_key, extent, cuts, -0.22, 0.18) if cuts else 1.0
    array = jax.random.normal(stream_key, extent, jnp.float32) * width * factor_of
    return jnp.minimum(jnp.maximum(array, -limit), limit).astype(held_as)


def setup_inputs(seed: int = 0) -> dict:
    splits = jax.random.split(jax.random.key(seed), 20)
    return {
        "skip_trunk_vector": draw_skip_trunk_vector(jax.random.fold_in(splits[19], 71), 0),
        "valve_preactivation": noise(splits[1], (SEQUENCE_SPAN, MIXING_WIDTH), 1.0, 6.0, ((0, 32), (1, 8))),
        "projected_heads_payload": noise(splits[2], (SEQUENCE_SPAN, MIXING_WIDTH), 1.0, 6.0, ((0, 32), (1, 8))),
        "cluster_ingests": noise(splits[3], (SEQUENCE_SPAN, GROUPS * STATE), 1.0, 6.0, ((0, 32), (1, 8))),
        "cluster_observers": noise(splits[4], (SEQUENCE_SPAN, GROUPS * STATE), 1.0, 6.0, ((0, 32), (1, 8))),
        "pre_softplus_increments": draw_pre_softplus_increments(jax.random.fold_in(splits[19], 71), 0),
        "attenuation_ln_rate": draw_attenuation_ln_rate(jax.random.fold_in(splits[19], 71), 0),
        "additional_attenuation": draw_additional_attenuation(jax.random.fold_in(splits[19], 71), 0),
        "payload_conv_weights": noise(splits[8], (CONV, MIXING_WIDTH), CONV ** -0.5, 2.0, ((1, 8),), jnp.float32),
        "ingest_conv_weights": noise(splits[9], (CONV, GROUPS * STATE), CONV ** -0.5, 2.0, ((1, 8),), jnp.float32),
        "observer_conv_weights": noise(splits[10], (CONV, GROUPS * STATE), CONV ** -0.5, 2.0, ((1, 8),), jnp.float32),
        "valved_cluster_factor": jnp.clip(1.0 + 0.18 * jax.random.normal(splits[11], (MIXING_WIDTH,), jnp.float32), 0.1, 1.9),
        "closing_map_matrix": noise(splits[12], (MIXING_WIDTH, D), MIXING_WIDTH ** -0.5, 0.125, ((0, 8),)),
        "dense_standardize_factor": jnp.clip(1.0 + 0.18 * jax.random.normal(splits[13], (D,), jnp.float32), 0.1, 1.9),
        "dense_valve_map": noise(splits[14], (D, FF), D ** -0.5, 0.125, ((0, 32), (1, 8))),
        "dense_payload_map": noise(splits[15], (D, FF), D ** -0.5, 0.125, ((0, 32), (1, 8))),
        "valve_series_smoother": noise(splits[16], (FF_TAPS, FF), FF_TAPS ** -0.5, 3.5, ((1, 8),), jnp.float32),
        "payload_series_smoother": noise(splits[17], (FF_TAPS, FF), FF_TAPS ** -0.5, 3.5, ((1, 8),), jnp.float32),
        "dense_contract_map": noise(splits[18], (FF, D), FF ** -0.5, 0.078125, ((0, 8), (1, 32))),
    }


EPSILON = 1e-06

def centred_conv(data, kernel):
    margin = kernel.shape[0] // 2
    length = data.shape[0]
    padded = jnp.pad(data, ((margin, margin), (0, 0)))
    summed = padded[0:length] * kernel[0]
    for offset in range(1, kernel.shape[0]):
        summed = summed + padded[offset:offset + length] * kernel[offset]
    return summed

def one_way(values_f, inputs_h, readout_h, stride_lengths_change, fading_exponent):
    blocks = SEQUENCE_SPAN // TOK_DEV
    places = jnp.arange(TOK_DEV, dtype=jnp.int32)
    lower_mask = places[:, None] >= places[None, :]

    def advance(carried, pieces):
        block_values, block_inputs, block_readout, block_steps, block_logs = pieces
        running = jnp.cumsum(block_logs, axis=0)
        log_gaps = running.T[:, :, None] - running.T[:, None, :]
        decays = jnp.exp(jnp.where(lower_mask[None], log_gaps, -jnp.inf))
        scores = jnp.einsum('thn,shn->hts', block_readout, block_inputs, precision=lax.Precision.HIGHEST)
        weights = scores * decays * block_steps.T[:, None, :]
        within = jnp.einsum('hts,shp->thp', weights, block_values, precision=lax.Precision.HIGHEST)
        outer = jnp.einsum('thn,hpn->thp', block_readout, carried, precision=lax.Precision.HIGHEST)
        outer = outer * jnp.exp(running)[:, :, None]
        to_end = jnp.exp(running[-1][None, :] - running) * block_steps
        block_state = jnp.einsum('sh,shp,shn->hpn', to_end, block_values, block_inputs, precision=lax.Precision.HIGHEST)
        carried = carried * jnp.exp(running[-1])[:, None, None] + block_state
        return (carried, within + outer)
    pieces = (values_f.reshape(blocks, TOK_DEV, HEADS, HEAD_DIM), inputs_h.reshape(blocks, TOK_DEV, HEADS, STATE), readout_h.reshape(blocks, TOK_DEV, HEADS, STATE), stride_lengths_change.reshape(blocks, TOK_DEV, HEADS), fading_exponent.reshape(blocks, TOK_DEV, HEADS))
    start_state = jnp.zeros((HEADS, HEAD_DIM, STATE), jnp.float32)
    final_state, results = lax.scan(advance, start_state, pieces)
    return results.reshape(SEQUENCE_SPAN, HEADS, HEAD_DIM)

def split_product(left, right, part_width, out_width):

    def add_part(summed, index):
        start = index * part_width
        columns = lax.dynamic_slice_in_dim(left, start, part_width, 1)
        rows_part = lax.dynamic_slice_in_dim(right, start, part_width, 0)
        term = jnp.dot(columns, rows_part, preferred_element_type=jnp.float32).astype(jnp.bfloat16)
        return (summed + lax.optimization_barrier(term).astype(jnp.float32), index)
    zero_sum = jnp.zeros((left.shape[0], out_width), jnp.float32)
    summed, indices = lax.scan(add_part, zero_sum, jnp.arange(N_TP, dtype=jnp.int32))
    return summed

def reference(skip_trunk_vector, valve_preactivation, projected_heads_payload, cluster_ingests, cluster_observers, pre_softplus_increments, attenuation_ln_rate, additional_attenuation, payload_conv_weights, ingest_conv_weights, observer_conv_weights, valved_cluster_factor, closing_map_matrix, dense_standardize_factor, dense_valve_map, dense_payload_map, valve_series_smoother, payload_series_smoother, dense_contract_map):
    per_group = HEADS // GROUPS
    mixed_values = jax.nn.silu(centred_conv(projected_heads_payload.astype(jnp.float32), payload_conv_weights)).astype(jnp.bfloat16)
    mixed_inputs = jax.nn.silu(centred_conv(cluster_ingests.astype(jnp.float32), ingest_conv_weights)).astype(jnp.bfloat16)
    mixed_readout = jax.nn.silu(centred_conv(cluster_observers.astype(jnp.float32), observer_conv_weights)).astype(jnp.bfloat16)
    values_f = mixed_values.astype(jnp.float32).reshape(SEQUENCE_SPAN, HEADS, HEAD_DIM)
    inputs_h = jnp.repeat(mixed_inputs.astype(jnp.float32).reshape(SEQUENCE_SPAN, GROUPS, STATE), per_group, axis=1)
    readout_h = jnp.repeat(mixed_readout.astype(jnp.float32).reshape(SEQUENCE_SPAN, GROUPS, STATE), per_group, axis=1)
    stride_lengths_change = jax.nn.softplus(pre_softplus_increments)
    fading_exponent = additional_attenuation - stride_lengths_change * jnp.exp(attenuation_ln_rate)[:, None, :]
    forward = one_way(values_f, inputs_h, readout_h, stride_lengths_change[0], fading_exponent[0])
    backward = jnp.flip(one_way(jnp.flip(values_f, 0), jnp.flip(inputs_h, 0), jnp.flip(readout_h, 0), jnp.flip(stride_lengths_change[1], 0), jnp.flip(fading_exponent[1], 0)), 0)
    gated = (forward + backward).reshape(SEQUENCE_SPAN, MIXING_WIDTH) * jax.nn.silu(valve_preactivation.astype(jnp.float32))
    grouped = gated.reshape(SEQUENCE_SPAN, GROUPS, MIXING_WIDTH // GROUPS)
    standardized = grouped * lax.rsqrt(lax.optimization_barrier(jnp.mean(grouped * grouped, axis=2, keepdims=True)) + EPSILON)
    blending_result = (standardized.reshape(SEQUENCE_SPAN, MIXING_WIDTH) * valved_cluster_factor).astype(jnp.bfloat16)
    mapped_vector = split_product(blending_result, closing_map_matrix, MIXING_WIDTH // N_TP, D)
    intermediate_hidden = (skip_trunk_vector.astype(jnp.float32) + mapped_vector).astype(jnp.bfloat16)
    middle_f = intermediate_hidden.astype(jnp.float32)
    scaled = middle_f * lax.rsqrt(lax.optimization_barrier(jnp.mean(middle_f * middle_f, axis=1, keepdims=True)) + EPSILON)
    normed_rows = (scaled * dense_standardize_factor).astype(jnp.bfloat16)
    gate_rows = jnp.dot(normed_rows, dense_valve_map, preferred_element_type=jnp.float32).astype(jnp.bfloat16)
    value_rows = jnp.dot(normed_rows, dense_payload_map, preferred_element_type=jnp.float32).astype(jnp.bfloat16)
    gate_conv = centred_conv(gate_rows.astype(jnp.float32), valve_series_smoother)
    value_conv = centred_conv(value_rows.astype(jnp.float32), payload_series_smoother)
    hidden = (jax.nn.silu(gate_conv) * value_conv).astype(jnp.bfloat16)
    down_sum = split_product(hidden, dense_contract_map, FF // N_TP, D)
    return (middle_f + down_sum).astype(jnp.bfloat16)
```

```python
import jax
import jax.numpy as jnp
from jax import lax
from jax.experimental import pallas as pl
from jax.experimental.pallas import tpu as pltpu
from jax.sharding import Mesh
from jax.sharding import PartitionSpec as P

EPSILON = 1e-06
MESH = pl.DeviceIdType.MESH
NZ, NY, NX = 8, 4, 4
NSP, NTP = NZ * NY, NX * 2
T = 512
CH = 128
HEAD = 64
W_ROWS = 64
ORDER = (0, 3, 1, 2)
F32, BF16 = jnp.float32, jnp.bfloat16


def silu(v):
    return v / (1.0 + jnp.exp(-v))


def layer(
    skip, valve, payload, ingest, observer, pre, rate, extra, taps_p, taps_i, taps_o,
    group_gain, closing, norm_gain, own_w, taps_g, taps_v, out,
    wbuf, wc, xpad, taps, vals, ins, outs, rows, cols, weights, inner,
    dec_src, dec_rcv, st_src, st_rcv, res_src, res_rcv, state_in,
    mix, mid, normed, gate, value, edge_src, edge_rcv, hidden,
    d2d_src, d2d_rcv, own_sum, far_src, far_rcv, near_src, near_rcv,
    s_w, s_small, s_ag,
    r_z, r_y, r_f, r_dy, r_dz, r_small, r_ag, r_d2d, r_far, r_near, s_tail,
):
    z, y = lax.axis_index("z"), lax.axis_index("y")
    x, c = lax.axis_index("x"), lax.axis_index("c")
    sp, tp = z * NY + y, x * 2 + c
    xl, xr, xo = lax.rem(x + 3, NX), lax.rem(x + 1, NX), lax.rem(x + 2, NX)
    zl, zr = lax.rem(z + 7, NZ), lax.rem(z + 1, NZ)
    yl, yr, yo = lax.rem(y + 3, NY), lax.rem(y + 1, NY), lax.rem(y + 2, NY)
    sib = {"c": 1 - c}
    nxt, prv = lax.rem(sp + 1, NSP), lax.rem(sp + NSP - 1, NSP)

    def at_sp(s):
        return {"z": s // NY, "y": lax.rem(s, NY)}

    def rc(src, dst, ssem, rsem, dev):
        return pltpu.make_async_remote_copy(
            src_ref=src, dst_ref=dst, send_sem=ssem, recv_sem=rsem, device_id=dev, device_id_type=MESH
        )

    def got(ref, rsem, dev):
        rc(ref, ref, s_w, rsem, dev).wait_recv()

    def sent(ref, ssem, dev):
        rc(ref, ref, ssem, r_d2d.at[0], dev).wait_send()

    def wrow(zi, yi):
        return pl.ds(pl.multiple_of((zi * NY + yi) * W_ROWS, W_ROWS), W_ROWS)

    def zoff(dz):
        return lax.rem(z + dz, NZ)

    def gv_z_send(k):
        if k == 0:
            a = b = own_w.at[0:2]
            da = db = wbuf.at[0:2, wrow(z, y)]
        else:
            lo, hi = wrow(zoff(8 - k), y), wrow(zoff(k), y)
            if k < 3:
                a = da = wbuf.at[0:2, lo]
                b = db = wbuf.at[0:2, hi]
            else:
                a = da = wbuf.at[0, lo]
                b = db = wbuf.at[1, hi]
        rc(a, da, s_w, r_z.at[0, k], {"z": zr}).start()
        rc(b, db, s_w, r_z.at[1, k], {"z": zl}).start()

    def gv_z_wait(k):
        lo, hi = wrow(zoff(7 - k), y), wrow(zoff(1 + k), y)
        if k < 3:
            got(wbuf.at[0:2, lo], r_z.at[0, k], {"z": zl})
            got(wbuf.at[0:2, hi], r_z.at[1, k], {"z": zr})
        else:
            got(wbuf.at[0, lo], r_z.at[0, k], {"z": zl})
            got(wbuf.at[1, hi], r_z.at[1, k], {"z": zr})

    def gv_y_send(dz):
        dst = wbuf.at[0:2, wrow(zoff(dz), y)]
        src = own_w.at[0:2] if dz == 0 else dst
        rc(src, dst, s_w, r_y.at[0, dz], {"y": yr}).start()
        rc(src, dst, s_w, r_y.at[1, dz], {"y": yl}).start()

    def gv_y_fwd(dz):
        lo, hi = wrow(zoff(dz), yl), wrow(zoff(dz), yr)
        got(wbuf.at[0:2, lo], r_y.at[0, dz], {"y": yl})
        rc(wbuf.at[0, lo], wbuf.at[0, lo], s_w, r_f.at[0, dz], {"y": yr}).start()
        got(wbuf.at[0:2, hi], r_y.at[1, dz], {"y": yr})
        rc(wbuf.at[1, hi], wbuf.at[1, hi], s_w, r_f.at[1, dz], {"y": yl}).start()

    def gv_f_wait(dz):
        far = wrow(zoff(dz), yo)
        got(wbuf.at[0, far], r_f.at[0, dz], {"y": yl})
        got(wbuf.at[1, far], r_f.at[1, dz], {"y": yr})

    def half(zi, yi, h):
        return pl.ds(pl.multiple_of((zi * NY + yi) * W_ROWS + h * 32, 32), 32)

    def dn_y_send():
        dst = wbuf.at[2, wrow(z, y)]
        rc(own_w.at[2], dst, s_w, r_dy.at[0], {"y": yr}).start()
        rc(own_w.at[2], dst, s_w, r_dy.at[1], {"y": yl}).start()

    def dn_y_fwd():
        got(wbuf.at[2, wrow(z, yl)], r_dy.at[0], {"y": yl})
        a = wbuf.at[2, half(z, yl, 0)]
        rc(a, a, s_w, r_dy.at[2], {"y": yr}).start()
        got(wbuf.at[2, wrow(z, yr)], r_dy.at[1], {"y": yr})
        b = wbuf.at[2, half(z, yr, 1)]
        rc(b, b, s_w, r_dy.at[3], {"y": yl}).start()

    def dn_y_wait():
        got(wbuf.at[2, half(z, yo, 0)], r_dy.at[2], {"y": yl})
        got(wbuf.at[2, half(z, yo, 1)], r_dy.at[3], {"y": yr})

    def drow(zi, h=None):
        if h is None:
            return pl.ds(pl.multiple_of(zi * 256, 256), 256)
        return pl.ds(pl.multiple_of(zi * 256 + h * 128, 128), 128)

    def dn_z_send(k):
        ha, hb = (None, None) if k < 3 else (0, 1)
        a = wbuf.at[2, drow(zoff((8 - k) % 8), ha)]
        b = wbuf.at[2, drow(zoff(k), hb)]
        rc(a, a, s_w, r_dz.at[0, k], {"z": zr}).start()
        rc(b, b, s_w, r_dz.at[1, k], {"z": zl}).start()

    def dn_z_wait(k):
        ha, hb = (None, None) if k < 3 else (0, 1)
        got(wbuf.at[2, drow(zoff(7 - k), ha)], r_dz.at[0, k], {"z": zl})
        got(wbuf.at[2, drow(zoff(1 + k), hb)], r_dz.at[1, k], {"z": zr})

    tl, tr, to = xl * 2 + c, xr * 2 + c, xo * 2 + c

    def ag_a(buf, a, r):
        own = buf.at[tp, pl.ds(r * CH, CH)]
        rc(own, own, s_ag.at[a], r_ag.at[a, r, 1], {"x": xr}).start()
        rc(own, own, s_ag.at[a], r_ag.at[a, r, 2], {"x": xl}).start()
        rc(own, own, s_ag.at[a], r_ag.at[a, r, 0], sib).start()

    def ag_b(buf, a, r):
        lo, hi = buf.at[tl, pl.ds(r * CH, CH)], buf.at[tr, pl.ds(r * CH, CH)]
        got(lo, r_ag.at[a, r, 1], {"x": xl})
        fa = buf.at[tl, pl.ds(r * CH, CH // 2)]
        rc(fa, fa, s_ag.at[a], r_ag.at[a, r, 3], {"x": xr}).start()
        rc(lo, lo, s_ag.at[a], r_ag.at[a, r, 5], sib).start()
        got(hi, r_ag.at[a, r, 2], {"x": xr})
        fb = buf.at[tr, pl.ds(r * CH + CH // 2, CH // 2)]
        rc(fb, fb, s_ag.at[a], r_ag.at[a, r, 4], {"x": xl}).start()
        rc(hi, hi, s_ag.at[a], r_ag.at[a, r, 6], sib).start()

    def ag_c(buf, a, r):
        got(buf.at[to, pl.ds(r * CH, CH // 2)], r_ag.at[a, r, 3], {"x": xl})
        got(buf.at[to, pl.ds(r * CH + CH // 2, CH // 2)], r_ag.at[a, r, 4], {"x": xr})
        far = buf.at[to, pl.ds(r * CH, CH)]
        rc(far, far, s_ag.at[a], r_ag.at[a, r, 7], sib).start()

    def ag_d(buf, a, r):
        for kind, xi in ((0, x), (5, xl), (6, xr), (7, xo)):
            got(buf.at[xi * 2 + 1 - c, pl.ds(r * CH, CH)], r_ag.at[a, r, kind], sib)

    barrier = pltpu.get_barrier_semaphore()

    @pl.loop(1, NSP)
    def _(k):
        pl.semaphore_signal(barrier, inc=1, device_id=at_sp(lax.rem(sp + k, NSP)), device_id_type=MESH)

    @pl.loop(1, NTP)
    def _(k):
        d = lax.rem(tp + k, NTP)
        pl.semaphore_signal(
            barrier, inc=1, device_id={"x": d // 2, "c": lax.rem(d, 2)}, device_id_type=MESH
        )

    sign = lax.broadcasted_iota(jnp.int32, (8, 1), 0)
    lane = lax.broadcasted_iota(jnp.int32, (8, T), 1)
    raw = pre[...]
    dt = jnp.maximum(raw, 0.0) + jnp.log1p(jnp.exp(-jnp.abs(raw)))
    decay = extra[...] - dt * jnp.exp(rate[...])
    run = decay
    shift = 1
    while shift < T:
        run = run + jnp.where(lane >= shift, pltpu.roll(run, shift, 1), 0.0)
        shift *= 2
    total = run[:, T - 1 : T]
    forward = sign < 4
    before = jnp.where(lane >= 1, pltpu.roll(run, 1, 1), 0.0)
    place = jnp.where(forward, run, before)
    rows[0:8] = place
    rows[8:16] = dt
    rows[16:24] = jnp.exp(jnp.where(forward, total - run, before)) * dt
    carry_scale = jnp.exp(jnp.where(forward, run, total - before))
    cols[...] = jnp.transpose(jnp.concatenate([place, carry_scale], axis=0), (1, 0))
    block_decay = jnp.exp(total)
    lane1 = lax.broadcasted_iota(jnp.int32, (1, 128), 1)
    for g in range(4):
        first = jnp.broadcast_to(block_decay[2 * g : 2 * g + 1], (1, 128))
        second = jnp.broadcast_to(block_decay[2 * g + 1 : 2 * g + 2], (1, 128))
        dec_src[g] = jnp.where(lane1 < HEAD, first, second)
    dec_rcv[sp] = dec_src[y]
    wbuf[:, wrow(z, y), :] = own_w[...]
    xpad[8 : T + 8, 0:256] = payload[...].astype(F32)
    xpad[8 : T + 8, 256:384] = ingest[...].astype(F32)
    xpad[8 : T + 8, 384:512] = observer[...].astype(F32)
    taps[0:7, 0:256] = taps_p[...]
    taps[0:7, 256:384] = taps_i[...]
    taps[0:7, 384:512] = taps_o[...]
    wc[tp] = closing[:, pl.ds(pl.multiple_of(tp * 256, 256), 256)]

    def conv_strip(r):
        base = pl.multiple_of(r * 16, 16)
        part = xpad[pl.ds(base, 32), :]
        acc = part[5:21] * taps[0:1]
        for i in range(1, 7):
            acc = acc + part[5 + i : 21 + i] * taps[i : i + 1]
        acc = silu(acc).astype(BF16)
        vals[pl.ds(base, 16), :] = acc[:, 0:256]
        ins[pl.ds(base, 16), :] = acc[:, 256:384]
        outs[pl.ds(base, 16), :] = acc[:, 384:512]

    pl.semaphore_wait(barrier, NSP - 1 + NTP - 1)

    rc(xpad.at[T : T + 8], xpad.at[0:8], s_small.at[0], r_small.at[0], at_sp(nxt)).start()
    rc(xpad.at[8:16], xpad.at[T + 8 : T + 16], s_small.at[1], r_small.at[1], at_sp(prv)).start()

    @pl.loop(1, NSP)
    def _(k):
        d = lax.rem(sp + k, NSP)
        rc(dec_src.at[lax.rem(d, NY)], dec_rcv.at[sp], s_small.at[2], r_small.at[2], at_sp(d)).start()

    gv_z_send(0)
    gv_y_send(0)
    dn_y_send()

    @pl.loop(1, NTP)
    def _(k):
        d = lax.rem(tp + k, NTP)
        src = closing.at[:, pl.ds(pl.multiple_of(d * 256, 256), 256)]
        rc(src, wc.at[tp], s_small.at[3], r_small.at[3], {"x": d // 2, "c": lax.rem(d, 2)}).start()

    @pl.loop(1, 31)
    def _(r):
        conv_strip(r)

    got(xpad.at[0:8], r_small.at[0], at_sp(prv))
    got(xpad.at[T + 8 : T + 16], r_small.at[1], at_sp(nxt))
    sent(xpad.at[T : T + 8], s_small.at[0], at_sp(nxt))
    sent(xpad.at[8:16], s_small.at[1], at_sp(prv))
    xpad[0:8] = xpad[0:8] * (sp > 0).astype(F32)
    xpad[T + 8 : T + 16] = xpad[T + 8 : T + 16] * (sp < NSP - 1).astype(F32)
    conv_strip(0)
    conv_strip(31)

    ins_t = jnp.transpose(ins[...].astype(F32), (1, 0))
    lanes = lax.broadcasted_iota(jnp.int32, (128, 128), 1)
    for g in range(4):
        pair = vals[:, (g % 2) * 128 : (g % 2) * 128 + 128]
        first = jnp.dot(
            (ins_t * rows[16 + 2 * g : 17 + 2 * g]).astype(BF16), pair, preferred_element_type=F32
        )
        second = jnp.dot(
            (ins_t * rows[17 + 2 * g : 18 + 2 * g]).astype(BF16), pair, preferred_element_type=F32
        )
        tile = jnp.where(lanes < HEAD, first, second).astype(BF16)
        for i in range(8):
            st_src[4 * i + g] = tile[16 * i : 16 * i + 16]
    st_rcv[sp] = st_src[sp]

    @pl.loop(1, NSP)
    def _(k):
        d = lax.rem(sp + k, NSP)
        rc(st_src.at[d], st_rcv.at[sp], s_small.at[4], r_small.at[4], at_sp(d)).start()

    gv_z_wait(0)
    gv_z_send(1)
    gv_y_send(7)
    gv_y_send(1)

    @pl.loop(0, T // CH)
    def _(tc):
        trows = pl.ds(pl.multiple_of(tc * CH, CH), CH)
        read_t = outs[trows, :]
        at_t = cols[trows, :]
        low = lax.broadcasted_iota(jnp.int32, (CH, CH), 0) - lax.broadcasted_iota(jnp.int32, (CH, CH), 1)
        for sc in range(T // CH):
            scol = slice(sc * CH, sc * CH + CH)
            score = lax.dot_general(
                read_t, ins[scol, :], (((1,), (1,)), ((), ())), preferred_element_type=F32
            )
            gap = low + (tc - sc) * CH
            for h in range(4):
                rf = rows[h : h + 1, scol]
                rb = rows[4 + h : 5 + h, scol]
                df = rows[8 + h : 9 + h, scol]
                db = rows[12 + h : 13 + h, scol]
                gaps = jnp.where(gap >= 0, at_t[:, h : h + 1] - rf, rb - at_t[:, 4 + h : 5 + h])
                step = jnp.where(gap > 0, df, jnp.where(gap < 0, db, df + db))
                weights[h, :, scol] = (score * jnp.exp(gaps) * step).astype(BF16)
        for p in range(2):
            pair = vals[:, p * 128 : p * 128 + 128]
            first = jnp.dot(weights[2 * p], pair, preferred_element_type=F32)
            second = jnp.dot(weights[2 * p + 1], pair, preferred_element_type=F32)
            inner[trows, p * 128 : p * 128 + 128] = jnp.where(lanes < HEAD, first, second)

    gv_y_fwd(0)
    dn_y_fwd()

    got(dec_rcv.at[0 : NSP - 1], r_small.at[2], at_sp(nxt))
    got(st_rcv.at[0 : NSP - 1], r_small.at[4], at_sp(nxt))
    back = y // 2
    carry = jnp.zeros((16, 128), F32)
    for k in range(NSP):
        at = k + back * (NSP - 1 - 2 * k)
        res_src[at] = carry.astype(BF16)
        carry = carry * dec_rcv[at] + st_rcv[at].astype(F32)
    res_rcv[sp] = res_src[sp]

    @pl.loop(1, NSP)
    def _(k):
        d = lax.rem(sp + k, NSP)
        rc(res_src.at[d], res_rcv.at[sp], s_small.at[5], r_small.at[5], at_sp(d)).start()

    gv_z_wait(1)
    gv_z_send(2)
    gv_y_send(6)
    gv_y_send(2)
    gv_y_fwd(7)
    gv_y_fwd(1)
    dn_y_wait()
    got(res_rcv.at[0 : NSP - 1], r_small.at[5], at_sp(nxt))
    for i in range(8):
        for g in range(4):
            state_in[16 * i : 16 * i + 16, 128 * g : 128 * g + 128] = res_rcv[4 * i + g]
    dn_z_send(0)

    for r in ORDER:
        rr = slice(r * CH, r * CH + CH)
        carried = jnp.dot(outs[rr, :], state_in[...], preferred_element_type=F32)
        at_t = cols[rr, :]
        parts = []
        for p in range(2):
            s0 = jnp.where(lanes < HEAD, at_t[:, 8 + 2 * p : 9 + 2 * p], at_t[:, 9 + 2 * p : 10 + 2 * p])
            s1 = jnp.where(lanes < HEAD, at_t[:, 12 + 2 * p : 13 + 2 * p], at_t[:, 13 + 2 * p : 14 + 2 * p])
            pc = slice(128 * p, 128 * p + 128)
            both = inner[rr, pc] + s0 * carried[:, pc] + s1 * carried[:, 256 + 128 * p : 384 + 128 * p]
            parts.append(both * silu(valve[rr, pc].astype(F32)))
        square = jnp.sum(parts[0] * parts[0] + parts[1] * parts[1], axis=1, keepdims=True)
        scale = lax.rsqrt(square * (1.0 / 256) + EPSILON)
        for p in range(2):
            pc = slice(128 * p, 128 * p + 128)
            mix[tp, rr, pc] = (parts[p] * scale * group_gain[0:1, pc]).astype(BF16)
        ag_a(mix, 0, r)

    got(wc.at[0 : NTP - 1], r_small.at[3], sib)

    def project(r):
        rr = slice(r * CH, r * CH + CH)
        acc = skip[rr, :].astype(F32)
        for j in range(NTP):
            acc = acc + jnp.dot(mix[j, rr, :], wc[j], preferred_element_type=F32)
        mid[tp, rr, :] = acc.astype(BF16)
        ag_a(mid, 1, r)

    def norm(n, r):
        @pl.loop(0, CH // 16)
        def _(q):
            rr = pl.ds(pl.multiple_of(r * CH + q * 16, 16), 16)
            square = jnp.zeros((16, 256), F32)
            for j in range(NTP):
                part = mid[j, rr, :].astype(F32)
                square = square + part * part
            scale = lax.rsqrt(jnp.sum(square, axis=1, keepdims=True) * (1.0 / 2048) + EPSILON)
            to_rows = pl.ds(pl.multiple_of(n * CH + q * 16, 16), 16)
            for j in range(NTP):
                jc = slice(256 * j, 256 * j + 256)
                normed[to_rows, jc] = (mid[j, rr, :].astype(F32) * scale * norm_gain[0:1, jc]).astype(BF16)

    r0, r1, r2, r3 = ORDER
    ag_b(mix, 0, r0)
    ag_b(mix, 0, r1)
    ag_c(mix, 0, r0)
    ag_d(mix, 0, r0)
    project(r0)
    gv_z_wait(2)
    gv_z_send(3)
    gv_y_send(5)
    gv_y_send(3)
    ag_b(mix, 0, r2)
    ag_c(mix, 0, r1)
    ag_d(mix, 0, r1)
    project(r1)
    gv_y_fwd(6)
    gv_y_fwd(2)
    ag_b(mix, 0, r3)
    ag_c(mix, 0, r2)
    ag_d(mix, 0, r2)
    project(r2)
    gv_z_wait(3)
    gv_y_send(4)
    dn_z_wait(0)
    dn_z_send(1)
    ag_b(mid, 1, r0)
    ag_c(mix, 0, r3)
    ag_d(mix, 0, r3)
    project(r3)
    gv_y_fwd(5)
    gv_y_fwd(3)
    ag_b(mid, 1, r1)
    ag_c(mid, 1, r0)
    ag_d(mid, 1, r0)
    norm(0, r0)
    ag_b(mid, 1, r2)
    ag_c(mid, 1, r1)
    ag_d(mid, 1, r1)
    norm(1, r1)
    dn_z_wait(1)
    dn_z_send(2)
    gv_y_fwd(4)
    ag_b(mid, 1, r3)
    ag_c(mid, 1, r2)
    ag_d(mid, 1, r2)
    norm(2, r2)
    ag_c(mid, 1, r3)
    ag_d(mid, 1, r3)
    norm(3, r3)
    for dz in range(8):
        gv_f_wait(dz)
    dn_z_wait(2)
    dn_z_send(3)

    def expand(n):
        rr = slice(n * 256, n * 256 + 256)
        for k, dst in ((0, gate), (1, value)):
            res = jnp.dot(normed[rr, :], wbuf[k], preferred_element_type=F32)
            for i in range(2):
                at = ORDER[2 * n + i] * CH + 8
                dst[at : at + CH, :] = res[i * CH : i * CH + CH]

    expand(0)
    edge_src[0, 0:1, :] = gate[T + 7 : T + 8, :]
    edge_src[0, 1:2, :] = value[T + 7 : T + 8, :]
    edge_src[1, 0:1, :] = gate[8:9, :]
    edge_src[1, 1:2, :] = value[8:9, :]
    rc(edge_src.at[0], edge_rcv.at[0], s_tail.at[0], r_small.at[6], at_sp(nxt)).start()
    rc(edge_src.at[1], edge_rcv.at[1], s_tail.at[1], r_small.at[7], at_sp(prv)).start()
    expand(1)

    def hidden_strip(r):
        base = pl.multiple_of(r * 16, 16)
        g, v = gate[pl.ds(base, 32), :], value[pl.ds(base, 32), :]
        gc = g[7:23] * taps_g[0:1] + g[8:24] * taps_g[1:2] + g[9:25] * taps_g[2:3]
        vc = v[7:23] * taps_v[0:1] + v[8:24] * taps_v[1:2] + v[9:25] * taps_v[2:3]
        hidden[pl.ds(base, 16), :] = (silu(gc) * vc).astype(BF16)

    @pl.loop(1, 31)
    def _(r):
        hidden_strip(r)

    got(edge_rcv.at[0], r_small.at[6], at_sp(prv))
    got(edge_rcv.at[1], r_small.at[7], at_sp(nxt))
    has_prv, has_nxt = (sp > 0).astype(F32), (sp < NSP - 1).astype(F32)
    gate[7:8, :] = edge_rcv[0, 0:1, :] * has_prv
    value[7:8, :] = edge_rcv[0, 1:2, :] * has_prv
    gate[T + 8 : T + 9, :] = edge_rcv[1, 0:1, :] * has_nxt
    value[T + 8 : T + 9, :] = edge_rcv[1, 1:2, :] * has_nxt
    hidden_strip(0)
    hidden_strip(31)
    dn_z_wait(3)

    def part_of(xi, ci):
        at = pl.multiple_of((xi * 2 + ci) * 256, 256)
        return lax.dot_general(
            hidden[...], wbuf[2, pl.ds(at, 256), :], (((1,), (1,)), ((), ())), preferred_element_type=F32
        )

    targets = (xo, xr, xl, x)
    for i in range(4):
        d2d_src[i] = part_of(targets[i], 1 - c).astype(BF16)
        rc(d2d_src.at[i], d2d_rcv.at[i], s_tail.at[2], r_d2d.at[i], sib).start()

    def chip_sum(i):
        own = part_of(targets[i], c)
        got(d2d_rcv.at[i], r_d2d.at[i], sib)
        return own + d2d_rcv[i].astype(F32)

    H = T // 2
    far_src[...] = chip_sum(0).astype(BF16)
    rc(far_src.at[0:H], far_rcv.at[0:H], s_tail.at[3], r_far.at[0], {"x": xr}).start()
    rc(far_src.at[H:T], far_rcv.at[H:T], s_tail.at[3], r_far.at[1], {"x": xl}).start()
    right = chip_sum(1)
    near_src[0, H:T] = right[H:T].astype(BF16)
    rc(near_src.at[0, H:T], near_rcv.at[0, H:T], s_tail.at[4], r_near.at[0], {"x": xr}).start()
    own_sum[0:H] = right[0:H]
    left = chip_sum(2)
    near_src[1, 0:H] = left[0:H].astype(BF16)
    rc(near_src.at[1, 0:H], near_rcv.at[1, 0:H], s_tail.at[4], r_near.at[1], {"x": xl}).start()
    own_sum[H:T] = left[H:T]
    got(far_rcv.at[0:H], r_far.at[0], {"x": xl})
    near_src[0, 0:H] = (own_sum[0:H] + far_rcv[0:H].astype(F32)).astype(BF16)
    rc(near_src.at[0, 0:H], near_rcv.at[0, 0:H], s_tail.at[4], r_near.at[2], {"x": xr}).start()
    got(far_rcv.at[H:T], r_far.at[1], {"x": xr})
    near_src[1, H:T] = (own_sum[H:T] + far_rcv[H:T].astype(F32)).astype(BF16)
    rc(near_src.at[1, H:T], near_rcv.at[1, H:T], s_tail.at[4], r_near.at[3], {"x": xl}).start()
    own_sum[...] = chip_sum(3) + mid[tp].astype(F32)
    got(near_rcv.at[0, H:T], r_near.at[0], {"x": xl})
    got(near_rcv.at[1, 0:H], r_near.at[1], {"x": xr})
    got(near_rcv.at[0, 0:H], r_near.at[2], {"x": xl})
    got(near_rcv.at[1, H:T], r_near.at[3], {"x": xr})
    out[...] = (own_sum[...] + near_rcv[0].astype(F32) + near_rcv[1].astype(F32)).astype(BF16)

    sent(dec_rcv.at[0 : NSP - 1], s_small.at[2], at_sp(nxt))
    sent(wc.at[0 : NTP - 1], s_small.at[3], sib)
    sent(st_rcv.at[0 : NSP - 1], s_small.at[4], at_sp(nxt))
    sent(res_rcv.at[0 : NSP - 1], s_small.at[5], at_sp(nxt))
    sent(wbuf.at[:, 0 : 31 * W_ROWS], s_w, {"z": zr})
    sent(mix.at[0:7], s_ag.at[0], sib)
    sent(mid.at[0:7], s_ag.at[1], sib)
    sent(edge_src.at[0], s_tail.at[0], at_sp(nxt))
    sent(edge_src.at[1], s_tail.at[1], at_sp(prv))
    sent(d2d_src, s_tail.at[2], sib)
    sent(far_src, s_tail.at[3], {"x": xr})
    sent(near_src, s_tail.at[4], {"x": xr})


def shards(
    skip, valve, payload, ingest, observer, pre, rate, extra, taps_p, taps_i, taps_o,
    group_gain, closing, norm_gain, w_gate, w_value, taps_g, taps_v, w_down,
):
    own_w = jnp.stack([w_gate, w_value, w_down.T])
    pre_r = jnp.transpose(pre, (0, 2, 1)).reshape(8, T)
    extra_r = jnp.transpose(extra, (0, 2, 1)).reshape(8, T)
    V, D = pltpu.VMEM, pltpu.SemaphoreType.DMA
    scratch = [
        V((3, 2048, 640), BF16),
        V((NTP, 256, 256), BF16),
        V((T + 16, 512), F32),
        V((8, 512), F32),
        V((T, 256), BF16),
        V((T, 128), BF16),
        V((T, 128), BF16),
        V((24, T), F32),
        V((T, 16), F32),
        V((4, CH, T), BF16),
        V((T, 256), F32),
        V((4, 1, 128), F32),
        V((NSP, 1, 128), F32),
        V((NSP, 16, 128), BF16),
        V((NSP, 16, 128), BF16),
        V((NSP, 16, 128), BF16),
        V((NSP, 16, 128), BF16),
        V((128, 512), BF16),
        V((NTP, T, 256), BF16),
        V((NTP, T, 256), BF16),
        V((T, 2048), BF16),
        V((T + 16, 640), F32),
        V((T + 16, 640), F32),
        V((2, 8, 640), F32),
        V((2, 8, 640), F32),
        V((T, 640), BF16),
        V((4, T, 256), BF16),
        V((4, T, 256), BF16),
        V((T, 256), F32),
        V((T, 256), BF16),
        V((T, 256), BF16),
        V((2, T, 256), BF16),
        V((2, T, 256), BF16),
        D,
        D((6,)),
        D((2,)),
        D((2, 4)),
        D((2, 8)),
        D((2, 8)),
        D((4,)),
        D((2, 4)),
        D((8,)),
        D((2, 4, 8)),
        D((4,)),
        D((2,)),
        D((4,)),
        D((5,)),
    ]
    return pl.pallas_call(
        layer,
        out_shape=jax.ShapeDtypeStruct((T, 256), BF16),
        in_specs=[pl.BlockSpec(memory_space=pltpu.VMEM)] * 17,
        out_specs=pl.BlockSpec(memory_space=pltpu.VMEM),
        scratch_shapes=scratch,
        compiler_params=pltpu.CompilerParams(
            collective_id=0, has_side_effects=True, vmem_limit_bytes=60 * 1024 * 1024
        ),
    )(
        skip, valve, payload, ingest, observer, pre_r, rate.reshape(8, 1), extra_r, taps_p, taps_i, taps_o,
        group_gain.reshape(1, 256), closing, norm_gain.reshape(1, 2048), own_w, taps_g, taps_v,
    )


def solution(mesh):
    finer = Mesh(mesh.devices.reshape(NZ, NY, NX, 2), ("z", "y", "x", "c"))
    SP, TP = ("z", "y"), ("x", "c")
    in_specs = (
        P(SP, TP),
        P(SP, TP),
        P(SP, TP),
        P(SP, TP),
        P(SP, TP),
        P(None, SP, TP),
        P(None, TP),
        P(None, SP, TP),
        P(None, TP),
        P(None, TP),
        P(None, TP),
        P(TP),
        P(TP, None),
        P(),
        P(SP, TP),
        P(SP, TP),
        P(None, TP),
        P(None, TP),
        P(TP, SP),
    )
    return jax.shard_map(
        shards, mesh=finer, in_specs=in_specs, out_specs=P(SP, TP), check_vma=False
    )
```
